32 devices in a mesh: sp: 4 (over x, core), tp: 8 (over z, y).
Axes of the slice: x: 2, y: 2, z: 4, core: 2. Of those that a mesh axis runs over, the one named last changes fastest.
Arguments:
- latents: bfloat16 [1024, 2048], P(('sp', 'tp')), may hold values from -6 to 6
- context: bfloat16 [256, 2048], P('sp'), may hold values from -6 to 6
- condition: float32 [2048], P('sp'), may hold values from -12 to 12
- context_condition: float32 [2048], P('sp'), may hold values from -12 to 12
- norm_gain: float32 [2048], replicated, may hold values from 0.1 to 1.9
- shift_weight: bfloat16 [2048, 2048], P('sp', 'tp'), may hold values from -0.09375 to 0.09375
- scale_weight: bfloat16 [2048, 2048], P('sp', 'tp'), may hold values from -0.09375 to 0.09375
- gate_weight: bfloat16 [2048, 2048], P('sp', 'tp'), may hold values from -0.125 to 0.125
- query_weight: bfloat16 [2048, 1024], P(None, 'tp'), may hold values from -0.125 to 0.125
- key_weight: bfloat16 [2048, 1024], P(None, 'tp'), may hold values from -0.125 to 0.125
- value_weight: bfloat16 [2048, 1024], P(None, 'tp'), may hold values from -0.125 to 0.125
- subtract_share: float32 [8], P('tp'), may hold values from 0.3 to 0.8
- head_gain: float32 [128], replicated, may hold values from 0.1 to 1.9
- output_weight: bfloat16 [1024, 2048], P('tp'), may hold values from -0.1875 to 0.1875
Outputs:
- updated: bfloat16 [1024, 2048], P(('sp', 'tp'))
The draws below stay inside these ranges and needn't reach their ends.
All inputs are finite; a program needn't handle non-finite values.
Results may differ from the reference program's by a relative error of at most 0.013.
Values may be sent and summed in bfloat16 or wider, within the bound.
No kernel may reach another device: no remote copies, remote signals or barrier semaphores. Data moves between devices by JAX's collectives and lax.ppermute only.
A program may use at most 64 MiB of HBM per device.

```python
import math
import jax
import jax.numpy as jnp
from jax import lax

D = 2048
HEAD = 64
VALUE = 128
HEADS = 8
GRID_W = 64
TOKENS = 1024
CTX = 256


def ramped_draw(base_key):
    position = jnp.arange(D, dtype=jnp.float32) / (D - 1)
    values = jnp.clip(jax.random.normal(base_key, (D,), jnp.float32), -4.0, 4.0)
    growth = jnp.exp(jnp.log(3.0) * position)
    return values * growth


def draw_condition(key, part):
    return ramped_draw(jax.random.fold_in(key, 11))


def draw_context_condition(key, part):
    return ramped_draw(jax.random.fold_in(key, 29))


def block_levels(key, shape, cuts, least, largest):
    def one(dim, shards_of):
        heights = jax.random.uniform(jax.random.fold_in(jax.random.fold_in(key, 6), dim), (shards_of,), jnp.float32, least / len(cuts), largest / len(cuts))
        return jnp.repeat(jnp.exp(heights), shape[dim] // shards_of).reshape((-1,) + (1,) * (len(shape) - dim - 1))

    level = one(*cuts[0])
    for cut in cuts[1:]:
        level = level * one(*cut)
    return level


def centred(rng, dims, spread, limit, cuts=(), kind=jnp.bfloat16):
    array = spread * jax.random.normal(rng, dims, jnp.float32)
    if cuts:
        array = array * block_levels(rng, dims, cuts, -0.22, 0.18)
    return jnp.clip(array, -limit, limit).astype(kind)


def setup_inputs(seed: int = 0) -> dict:
    streams_of = jax.random.split(jax.random.key(seed), 15)
    latents = centred(streams_of[0], (TOKENS, D), 1.0, 6.0, ((0, 32),))
    context = centred(streams_of[1], (CTX, D), 1.0, 6.0, ((0, 4),))
    condition = draw_condition(jax.random.fold_in(streams_of[14], 71), 0)
    context_condition = draw_context_condition(jax.random.fold_in(streams_of[14], 71), 0)
    norm_gain = jnp.clip(1.0 + 0.18 * jax.random.normal(streams_of[4], (D,), jnp.float32), 0.1, 1.9)
    shift_weight = centred(streams_of[5], (D, D), (2 * D) ** -0.5, 0.09375, ((0, 4), (1, 8)))
    scale_weight = centred(streams_of[6], (D, D), (2 * D) ** -0.5, 0.09375, ((0, 4), (1, 8)))
    gate_weight = centred(streams_of[7], (D, D), D ** -0.5, 0.125, ((0, 4), (1, 8)))
    query_weight = centred(streams_of[8], (D, HEADS * VALUE), D ** -0.5, 0.125, ((1, 8),))
    key_weight = centred(streams_of[9], (D, HEADS * VALUE), D ** -0.5, 0.125, ((1, 8),))
    value_weight = centred(streams_of[10], (D, HEADS * VALUE), D ** -0.5, 0.125, ((1, 8),))
    subtract_share = jnp.clip(0.3 + 0.5 * jax.random.uniform(streams_of[11], (HEADS,), jnp.float32) ** block_levels(streams_of[11], (HEADS,), ((0, 8),), -0.2, 0.2), 0.3, 0.8)
    head_gain = jnp.clip(1.0 + 0.18 * jax.random.normal(streams_of[12], (VALUE,), jnp.float32), 0.1, 1.9)
    output_weight = centred(streams_of[13], (HEADS * VALUE, D), (HEADS * VALUE) ** -0.5, 0.1875, ((0, 8),))
    return dict(latents=latents, context=context, condition=condition, context_condition=context_condition, norm_gain=norm_gain, shift_weight=shift_weight, scale_weight=scale_weight, gate_weight=gate_weight, query_weight=query_weight, key_weight=key_weight, value_weight=value_weight, subtract_share=subtract_share, head_gain=head_gain, output_weight=output_weight)


norm_eps = 1e-06
head_eps = 1e-05
rope_theta = 10000.0
head_scale = 0.8

def rotary_tables(positions):
    quarter = HEAD // 4
    inverse = rope_theta ** (-2.0 * jnp.arange(quarter, dtype=jnp.float32) / (HEAD // 2))
    row_angle = (positions // GRID_W).astype(jnp.float32)[:, None] * inverse[None, :]
    column_angle = (positions % GRID_W).astype(jnp.float32)[:, None] * inverse[None, :]
    angles = jnp.concatenate([row_angle, row_angle, column_angle, column_angle], axis=-1)
    return (jnp.cos(angles), jnp.sin(angles))

def rotate(vectors, cosine, sine_table):
    quarter = HEAD // 4
    pieces = vectors.reshape(vectors.shape[:-1] + (2, 2, quarter))
    turned = jnp.concatenate([-pieces[..., 1:, :], pieces[..., :1, :]], axis=-2).reshape(vectors.shape)
    return vectors * cosine[:, None, :] + turned * sine_table[:, None, :]

def modulate(token_rows, gain_row, shift_row, scale_row):
    widened = token_rows.astype(jnp.float32)
    normed = widened * lax.rsqrt(lax.optimization_barrier(jnp.mean(widened * widened, axis=-1, keepdims=True)) + norm_eps)
    return (normed * gain_row * (1.0 + scale_row) + shift_row).astype(jnp.bfloat16)

def differential(queries, key_value_rows, share_value, head_gain):
    ratios = []
    for which_map in range(2):
        offset = which_map * HEAD
        scores = jnp.dot(queries[:, offset:offset + HEAD], key_value_rows[:, offset:offset + HEAD].T, preferred_element_type=jnp.float32) * HEAD ** (-0.5)
        powers = jnp.exp(scores)
        weighted = jnp.dot(powers.astype(jnp.bfloat16), key_value_rows[:, VALUE:], preferred_element_type=jnp.float32)
        ratios.append(weighted / lax.optimization_barrier(jnp.sum(powers, axis=1, keepdims=True)))
    difference = ratios[0] - share_value * ratios[1]
    normed = difference * lax.rsqrt(lax.optimization_barrier(jnp.mean(difference * difference, axis=1, keepdims=True)) + head_eps)
    return (normed * head_gain * head_scale).astype(jnp.bfloat16)

def reference(latents, context, condition, context_condition, norm_gain, shift_weight, scale_weight, gate_weight, query_weight, key_weight, value_weight, subtract_share, head_gain, output_weight):
    activated = jax.nn.silu(jnp.stack([condition, context_condition])).astype(jnp.bfloat16)
    shift_terms = jnp.dot(activated, shift_weight, preferred_element_type=jnp.float32)
    scale_terms = jnp.dot(activated, scale_weight, preferred_element_type=jnp.float32)
    gate_terms = jnp.dot(activated, gate_weight, preferred_element_type=jnp.float32)
    latent_mod = modulate(latents, norm_gain, shift_terms[0], scale_terms[0])
    context_mod = modulate(context, norm_gain, shift_terms[1], scale_terms[1])
    cosine, sine_table = rotary_tables(jnp.arange(TOKENS, dtype=jnp.int32))
    block_rows = math.gcd(TOKENS, 512)

    def add_head(head_index, running):
        first_column = jnp.asarray(head_index, jnp.int32) * VALUE

        def columns(weight):
            return lax.dynamic_slice_in_dim(weight, first_column, VALUE, 1)
        latent_query = jnp.dot(latent_mod, columns(query_weight), preferred_element_type=jnp.float32)
        queries = rotate(latent_query.reshape(TOKENS, 2, HEAD), cosine, sine_table)
        queries = queries.reshape(TOKENS, VALUE).astype(jnp.bfloat16)
        latent_key = jnp.dot(latent_mod, columns(key_weight), preferred_element_type=jnp.float32)
        latent_keys = rotate(latent_key.reshape(TOKENS, 2, HEAD), cosine, sine_table)
        latent_keys = latent_keys.reshape(TOKENS, VALUE).astype(jnp.bfloat16)
        latent_values = jnp.dot(latent_mod, columns(value_weight), preferred_element_type=jnp.float32).astype(jnp.bfloat16)
        context_keys = jnp.dot(context_mod, columns(key_weight), preferred_element_type=jnp.float32).astype(jnp.bfloat16)
        context_values = jnp.dot(context_mod, columns(value_weight), preferred_element_type=jnp.float32).astype(jnp.bfloat16)
        key_value_rows = jnp.concatenate([jnp.concatenate([context_keys, context_values], axis=1), jnp.concatenate([latent_keys, latent_values], axis=1)], axis=0)
        share_value = lax.dynamic_index_in_dim(subtract_share, jnp.asarray(head_index, jnp.int32), 0, keepdims=False)

        def one_block(query_block):
            return differential(query_block, key_value_rows, share_value, head_gain)
        head_output = lax.map(one_block, queries.reshape(TOKENS // block_rows, block_rows, VALUE))
        head_output = head_output.reshape(TOKENS, VALUE)
        output_rows = lax.dynamic_slice_in_dim(output_weight, first_column, VALUE, 0)
        return running + jnp.dot(head_output, output_rows, preferred_element_type=jnp.float32)
    branch = lax.fori_loop(0, HEADS, add_head, jnp.zeros((TOKENS, D), jnp.float32))
    return (latents.astype(jnp.float32) + gate_terms[0] * branch).astype(jnp.bfloat16)
```

```python
import jax
import jax.numpy as jnp
from jax import lax
from jax.sharding import PartitionSpec as P

HEAD = 64
VALUE = 128
GRID_W = 64


norm_eps = 1e-06
head_eps = 1e-05
rope_theta = 10000.0
head_scale = 0.8


def rotary_tables(positions):
    quarter = HEAD // 4
    inverse = rope_theta ** (-2.0 * jnp.arange(quarter, dtype=jnp.float32) / (HEAD // 2))
    row_angle = (positions // GRID_W).astype(jnp.float32)[:, None] * inverse[None, :]
    column_angle = (positions % GRID_W).astype(jnp.float32)[:, None] * inverse[None, :]
    angles = jnp.concatenate([row_angle, row_angle, column_angle, column_angle], axis=-1)
    return (jnp.cos(angles), jnp.sin(angles))


def rotate(vectors, cosine, sine_table):
    quarter = HEAD // 4
    pieces = vectors.reshape(vectors.shape[:-1] + (2, 2, quarter))
    turned = jnp.concatenate([-pieces[..., 1:, :], pieces[..., :1, :]], axis=-2).reshape(
        vectors.shape
    )
    return vectors * cosine[:, None, :] + turned * sine_table[:, None, :]


def modulate(token_rows, gain_row, shift_row, scale_row):
    widened = token_rows.astype(jnp.float32)
    normed = widened * lax.rsqrt(jnp.mean(widened * widened, axis=-1, keepdims=True) + norm_eps)
    return (normed * gain_row * (1.0 + scale_row) + shift_row).astype(jnp.bfloat16)


def make_shards(sp_size, tp_size):
    y_size = 2 ** ((tp_size.bit_length() - 1) // 2)
    z_size = tp_size // y_size

    def z_shift(value, k):
        if k % z_size == 0:
            return value
        pairs = [
            (z * y_size + y, ((z + k) % z_size) * y_size + y)
            for z in range(z_size)
            for y in range(y_size)
        ]
        return lax.ppermute(value, "tp", pairs)

    def y_shift(value, j):
        if j % y_size == 0:
            return value
        pairs = [
            (z * y_size + y, z * y_size + (y + j) % y_size)
            for z in range(z_size)
            for y in range(y_size)
        ]
        return lax.ppermute(value, "tp", pairs)

    def core_swap(value):
        return lax.ppermute(value, "sp", [(i, i ^ 1) for i in range(sp_size)])

    def shards(
        latents,
        context,
        condition,
        context_condition,
        norm_gain,
        shift_weight,
        scale_weight,
        gate_weight,
        query_weight,
        key_weight,
        value_weight,
        subtract_share,
        head_gain,
        output_weight,
    ):
        rows = latents.shape[0]
        sp_index = lax.axis_index("sp")
        tp_index = lax.axis_index("tp")
        z_index, y_index = tp_index // y_size, tp_index % y_size
        core = sp_index % 2

        along_z = [z_shift(latents, k) for k in range(z_size)]
        chunks = [[y_shift(held, j) for j in range(y_size)] for held in along_z]

        activated = jax.nn.silu(jnp.stack([condition, context_condition])).astype(jnp.bfloat16)
        partial_terms = jnp.concatenate(
            [
                jnp.dot(activated, shift_weight, preferred_element_type=jnp.float32),
                jnp.dot(activated, scale_weight, preferred_element_type=jnp.float32),
                jnp.dot(activated[:1], gate_weight, preferred_element_type=jnp.float32),
            ],
            axis=0,
        )
        terms = partial_terms.shape[0]
        received = lax.all_to_all(
            jnp.broadcast_to(partial_terms, (sp_size * tp_size,) + partial_terms.shape),
            ("sp", "tp"),
            split_axis=0,
            concat_axis=0,
        )
        full_terms = jnp.sum(received.reshape((sp_size, tp_size) + partial_terms.shape), axis=0)
        full_terms = full_terms.transpose(1, 0, 2).reshape(terms, -1)

        half = VALUE // 2
        my_half = lax.dynamic_slice_in_dim(output_weight, core * half, half, 0)
        other_half = lax.dynamic_slice_in_dim(output_weight, (1 - core) * half, half, 0)
        fetched = [z_shift(my_half, -k) for k in range(1, z_size)]
        shared = [core_swap(piece) for piece in fetched]
        weight_pieces = [my_half, other_half]
        for mine, other in zip(fetched, shared):
            weight_pieces += [mine, other]
        tall_weight = jnp.concatenate(weight_pieces, axis=0)

        pair_weight = jnp.concatenate([key_weight, value_weight], axis=1)
        joined = jnp.concatenate([query_weight, pair_weight], axis=1)
        gathered = jnp.concatenate([chunks[k][j] for k in range(z_size) for j in range(y_size)])
        projected = jnp.dot(
            modulate(gathered, norm_gain, full_terms[0], full_terms[2]),
            joined,
            preferred_element_type=jnp.float32,
        )
        local_count = projected.shape[0]
        shift_k = jnp.arange(local_count, dtype=jnp.int32) // (y_size * rows)
        shift_j = (jnp.arange(local_count, dtype=jnp.int32) // rows) % y_size
        source_z = (z_index - shift_k) % z_size
        source_y = (y_index - shift_j) % y_size
        block = (sp_index * z_size + source_z) * y_size + source_y
        positions = block * rows + jnp.arange(local_count, dtype=jnp.int32) % rows
        cosine, sine_table = rotary_tables(positions)
        queries = rotate(projected[:, :VALUE].reshape(local_count, 2, HEAD), cosine, sine_table)
        queries = queries.reshape(local_count, VALUE).astype(jnp.bfloat16)
        latent_keys = rotate(
            projected[:, VALUE : 2 * VALUE].reshape(local_count, 2, HEAD), cosine, sine_table
        )
        latent_keys = latent_keys.reshape(local_count, VALUE).astype(jnp.bfloat16)
        latent_pairs = jnp.concatenate(
            [latent_keys, projected[:, 2 * VALUE :].astype(jnp.bfloat16)], axis=1
        )
        context_mod = modulate(context, norm_gain, full_terms[1], full_terms[3])
        context_pairs = jnp.dot(
            context_mod, pair_weight, preferred_element_type=jnp.float32
        ).astype(jnp.bfloat16)
        sent_pairs = jnp.concatenate([latent_pairs, context_pairs], axis=0)
        arrived = lax.all_gather(sent_pairs, "sp", axis=0, tiled=True)
        ratios = []
        for which_map in range(2):
            offset = which_map * HEAD
            scores = jnp.einsum(
                "qd,kd->qk",
                queries[:, offset : offset + HEAD],
                arrived[:, offset : offset + HEAD],
                preferred_element_type=jnp.float32,
            ) * HEAD ** (-0.5)
            powers = jnp.exp(scores)
            weighted = jnp.dot(
                powers.astype(jnp.bfloat16), arrived[:, VALUE:], preferred_element_type=jnp.float32
            )
            ratios.append(weighted / jnp.sum(powers, axis=1, keepdims=True))
        difference = ratios[0] - subtract_share[0] * ratios[1]
        normed = difference * lax.rsqrt(
            jnp.mean(difference * difference, axis=1, keepdims=True) + head_eps
        )
        head_output = (normed * head_gain * head_scale).astype(jnp.bfloat16)

        head_output = jnp.where(core == 0, head_output, jnp.roll(head_output, half, axis=1))
        wide = y_size * rows
        pieces = [z_shift(head_output[k * wide : (k + 1) * wide], -k) for k in range(z_size)]
        branch = jnp.dot(
            jnp.concatenate(pieces, axis=1), tall_weight, preferred_element_type=jnp.float32
        )
        total = branch[:rows]
        for j in range(1, y_size):
            sent = branch[j * rows : (j + 1) * rows].astype(jnp.bfloat16)
            total = total + y_shift(sent, -j).astype(jnp.float32)
        return (latents.astype(jnp.float32) + full_terms[4] * total).astype(jnp.bfloat16)

    return shards


def solution(mesh):
    in_specs = (
        P(("sp", "tp"), None),
        P("sp", None),
        P("sp"),
        P("sp"),
        P(),
        P("sp", "tp"),
        P("sp", "tp"),
        P("sp", "tp"),
        P(None, "tp"),
        P(None, "tp"),
        P(None, "tp"),
        P("tp"),
        P(),
        P("tp", None),
    )
    out_specs = P(("sp", "tp"), None)
    shards = make_shards(mesh.shape["sp"], mesh.shape["tp"])
    return jax.shard_map(shards, mesh=mesh, in_specs=in_specs, out_specs=out_specs, check_vma=False)
```

```python
import functools

import jax
import jax.numpy as jnp
from jax import lax
from jax.experimental import pallas as pl
from jax.experimental.pallas import tpu as pltpu
from jax.sharding import PartitionSpec as P

HEAD = 64
VALUE = 128
GRID_W = 64


norm_eps = 1e-06
head_eps = 1e-05
rope_theta = 10000.0
head_scale = 0.8


VMEM = pl.BlockSpec(memory_space=pltpu.VMEM)
SMEM = pl.BlockSpec(memory_space=pltpu.SMEM)
ANY = pl.BlockSpec(memory_space=pl.ANY)
PARAMS = pltpu.CompilerParams(vmem_limit_bytes=32 * 1024 * 1024)


def rotary_tables(positions):
    quarter = HEAD // 4
    lane = jnp.arange(VALUE, dtype=jnp.int32)[None, :]
    inverse = rope_theta ** (
        -2.0 * (lane % quarter).astype(jnp.float32) / (HEAD // 2)
    )
    place = jnp.where(
        lane % HEAD < HEAD // 2, positions[:, None] // GRID_W, positions[:, None] % GRID_W
    )
    angles = place.astype(jnp.float32) * inverse
    sine = jnp.sin(angles)
    ahead = lane % (2 * quarter) < quarter
    return jnp.cos(angles), jnp.where(ahead, -sine, 0.0), jnp.where(ahead, 0.0, sine)


def terms_kernel(condition, context_condition, shift, scale, gate, out):
    row = lax.broadcasted_iota(jnp.int32, (8, condition.shape[1]), 0)
    value = jnp.where(row == 0, condition[...], jnp.where(row == 1, context_condition[...], 0.0))
    activated = (value / (1.0 + jnp.exp(-value))).astype(jnp.bfloat16)
    shifts, scales, gates = (
        jnp.dot(activated, matrix[...], preferred_element_type=jnp.float32)
        for matrix in (shift, scale, gate)
    )
    lines = [shifts[:2], scales[:2], gates[:1]]
    out[...] = jnp.broadcast_to(jnp.concatenate(lines, axis=0)[None], out.shape)


def modulated(rows, gain, shift, scale):
    wide = rows.astype(jnp.float32)
    mean = jnp.mean(wide * wide, axis=-1, keepdims=True)
    normed = wide * lax.rsqrt(mean + norm_eps)
    return (normed * gain * (1.0 + scale) + shift).astype(jnp.bfloat16)


def project_kernel(count, with_context, *refs):
    pieces, refs = refs[:count], refs[count:]
    if with_context:
        context, refs = refs[0], refs[1:]
    terms, gain, query, key, value, cosine, ahead, behind, queries, pairs = refs
    gain_row = gain[...]
    rows = jnp.concatenate(
        [modulated(piece[...], gain_row, terms[0:1], terms[2:3]) for piece in pieces], axis=0
    )
    n = rows.shape[0]
    cos, sin_ahead, sin_behind = cosine[...], ahead[...], behind[...]

    def project(inputs, weight):
        return jnp.dot(inputs, weight[...], preferred_element_type=jnp.float32)

    def rotate(u):
        return (
            u * cos
            + pltpu.roll(u, VALUE - HEAD // 4, 1) * sin_ahead
            + pltpu.roll(u, HEAD // 4, 1) * sin_behind
        )

    queries[...] = (rotate(project(rows, query)) * HEAD ** (-0.5)).astype(jnp.bfloat16)
    pairs[:n, :VALUE] = rotate(project(rows, key)).astype(jnp.bfloat16)
    pairs[:n, VALUE:] = project(rows, value).astype(jnp.bfloat16)
    if with_context:
        extra = modulated(context[...], gain_row, terms[1:2], terms[3:4])
        pairs[n:, :VALUE] = project(extra, key).astype(jnp.bfloat16)
        pairs[n:, VALUE:] = project(extra, value).astype(jnp.bfloat16)


def attention_kernel(query_count, pair_count, *refs):
    queries, refs = refs[:query_count], refs[query_count:]
    pairs, refs = refs[:pair_count], refs[pair_count:]
    share, gain, out = refs
    query = jnp.concatenate([piece[...] for piece in queries], axis=0)
    n = query.shape[0]
    lane = lax.broadcasted_iota(jnp.int32, query.shape, 1)
    zero = jnp.zeros_like(query)
    stacked = jnp.concatenate(
        [jnp.where(lane < HEAD, query, zero), jnp.where(lane < HEAD, zero, query)], axis=0
    )
    sums = jnp.zeros((2 * n, VALUE), jnp.float32)
    totals = jnp.zeros((2 * n, 1), jnp.float32)
    for piece in pairs:
        powers = jnp.exp(
            lax.dot_general(
                stacked,
                piece[:, :VALUE],
                (((1,), (1,)), ((), ())),
                preferred_element_type=jnp.float32,
            )
        )
        totals = totals + jnp.sum(powers, axis=1, keepdims=True)
        sums = sums + jnp.dot(
            powers.astype(jnp.bfloat16), piece[:, VALUE:], preferred_element_type=jnp.float32
        )
    ratios = sums / totals
    difference = ratios[:n] - share[0] * ratios[n:]
    mean = jnp.mean(difference * difference, axis=1, keepdims=True)
    out[...] = (
        difference * lax.rsqrt(mean + head_eps) * gain[...] * head_scale
    ).astype(jnp.bfloat16)


def branch_kernel(ways, heads, rows, *refs):
    place, refs = refs[0], refs[1:]
    pieces, refs = refs[:heads], refs[heads:]
    weights, refs = refs[: heads * ways], refs[heads * ways :]
    own, sent = refs
    inputs = jnp.concatenate([piece[...] for piece in pieces], axis=1)
    width = own.shape[1] // ways
    for way in range(ways):
        part = None
        for head in range(heads):
            term = jnp.dot(
                inputs[:, head * VALUE : (head + 1) * VALUE],
                weights[head * ways + way][...],
                preferred_element_type=jnp.float32,
            )
            part = term if part is None else part + term
        columns = pl.ds(pl.multiple_of(place[way] * width, width), width)
        own[:, columns] = part[:rows]
        sent[:, columns] = part[rows:].astype(jnp.bfloat16)


def slice_kernel(place, weight, anchor, out):
    width = out.shape[1]
    out[...] = weight[:, pl.ds(pl.multiple_of(place[0] * width, width), width)]


def call(kernel, outs, ins, specs=None, flops=0, name=None):
    shapes = [jax.ShapeDtypeStruct(*out) for out in outs]
    single = len(shapes) == 1
    return pl.pallas_call(
        kernel,
        out_shape=shapes[0] if single else shapes,
        in_specs=specs or [VMEM] * len(ins),
        out_specs=VMEM if single else [VMEM] * len(shapes),
        compiler_params=PARAMS,
        cost_estimate=pl.CostEstimate(flops=flops, bytes_accessed=0, transcendentals=0),
        name=name,
    )(*ins)


def make_shards(sp_size, tp_size):
    y_size = 2 ** ((tp_size.bit_length() - 1) // 2)
    z_size = tp_size // y_size
    x_size = sp_size // 2
    ways = 4 if sp_size % 4 == 0 else 2
    bf16, f32 = jnp.bfloat16, jnp.float32

    def z_shift(value, k):
        if k % z_size == 0:
            return value
        pairs = [
            (z * y_size + y, ((z + k) % z_size) * y_size + y)
            for z in range(z_size)
            for y in range(y_size)
        ]
        return lax.ppermute(value, "tp", pairs)

    def y_shift(value, j):
        if j % y_size == 0:
            return value
        pairs = [
            (z * y_size + y, z * y_size + (y + j) % y_size)
            for z in range(z_size)
            for y in range(y_size)
        ]
        return lax.ppermute(value, "tp", pairs)

    def sp_swap(value, bit):
        return lax.ppermute(value, "sp", [(i, i ^ bit) for i in range(sp_size)])

    def x_shift(value, k):
        pairs = [
            (x * 2 + c, ((x + k) % x_size) * 2 + c) for x in range(x_size) for c in range(2)
        ]
        return lax.ppermute(value, "sp", pairs)

    def spread(value):
        pieces = [value, sp_swap(value, 1)]
        for k in range(1, x_size):
            piece = x_shift(value, k)
            pieces += [piece, sp_swap(piece, 1)]
        return pieces

    def shards(
        latents,
        context,
        condition,
        context_condition,
        norm_gain,
        shift_weight,
        scale_weight,
        gate_weight,
        query_weight,
        key_weight,
        value_weight,
        subtract_share,
        head_gain,
        output_weight,
    ):
        rows, width = latents.shape
        sp_index = lax.axis_index("sp")
        tp_index = lax.axis_index("tp")
        z_index, y_index = tp_index // y_size, tp_index % y_size

        chunks = {(0, 0): latents}
        for j in range(1, y_size):
            chunks[0, j] = y_shift(latents, j)
        for k in range(1, z_size):
            chunks[k, 0] = z_shift(latents, k)
        for k in range(1, z_size):
            for j in range(1, y_size):
                chunks[k, j] = y_shift(chunks[k, 0], j)

        devices = sp_size * tp_size
        columns = shift_weight.shape[1]
        partial_terms = call(
            terms_kernel,
            [((devices, 5, columns), f32)],
            [
                condition[None],
                context_condition[None],
                shift_weight,
                scale_weight,
                gate_weight,
            ],
            flops=3 * 16 * shift_weight.shape[0] * columns,
            name="terms",
        )
        received = lax.all_to_all(partial_terms, ("sp", "tp"), split_axis=0, concat_axis=0)
        full_terms = jnp.sum(received.reshape(sp_size, tp_size, 5, columns), axis=0)
        full_terms = full_terms.transpose(1, 0, 2).reshape(5, -1)

        quarter = width // ways
        low = sp_index % ways
        place = jnp.stack([low ^ bit for bit in range(ways)]).astype(jnp.int32)
        mine = call(
            slice_kernel,
            [((VALUE, quarter), bf16)],
            [place, output_weight, chunks[z_size // 2, 0]],
            [SMEM, VMEM, ANY],
            name="cut",
        )
        fetched = {k: z_shift(mine, -k) for k in range(1, z_size)}
        weights = []
        for k in range(z_size):
            if k == 0:
                by_way = [
                    lax.dynamic_slice_in_dim(output_weight, (low ^ bit) * quarter, quarter, 1)
                    for bit in range(ways)
                ]
            else:
                by_way = [fetched[k], sp_swap(fetched[k], 1)]
                if ways == 4:
                    across = sp_swap(fetched[k], 2)
                    by_way += [across, sp_swap(across, 1)]
            weights += by_way

        def project(keys, extra):
            pieces = [chunks[key] for key in keys]
            if rows % 16:
                pieces = [jnp.concatenate(pieces, axis=0)]
            count = len(keys) * rows
            shift_k, shift_j = (
                jnp.repeat(jnp.array([key[part] for key in keys], jnp.int32), rows)
                for part in range(2)
            )
            source_z = (z_index - shift_k) % z_size
            source_y = (y_index - shift_j) % y_size
            block = (sp_index * z_size + source_z) * y_size + source_y
            positions = block * rows + jnp.arange(count, dtype=jnp.int32) % rows
            total = count + sum(item.shape[0] for item in extra)
            return call(
                functools.partial(project_kernel, len(pieces), bool(extra)),
                [((count, VALUE), bf16), ((total, 2 * VALUE), bf16)],
                [
                    *pieces,
                    *extra,
                    full_terms,
                    norm_gain[None],
                    query_weight,
                    key_weight,
                    value_weight,
                    *rotary_tables(positions),
                ],
                flops=2 * count * width * 3 * VALUE,
                name="project",
            )

        first = [(k, 0) for k in range(z_size)]
        second = [(k, j) for j in range(1, y_size) for k in range(z_size)]
        queries_a, pairs_a = project(first, [context])
        arrived = spread(pairs_a)
        queries = [queries_a]
        if second:
            queries_b, pairs_b = project(second, [])
            queries.append(queries_b)
            arrived += spread(pairs_b)
        head_output = call(
            functools.partial(attention_kernel, len(queries), len(arrived)),
            [((sum(q.shape[0] for q in queries), VALUE), bf16)],
            [*queries, *arrived, subtract_share, head_gain[None]],
            [VMEM] * (len(queries) + len(arrived)) + [SMEM, VMEM],
            flops=8 * queries[0].shape[0] * VALUE * sum(p.shape[0] for p in arrived),
            name="attention",
        )

        by_block = head_output.reshape(y_size, z_size, rows, VALUE)
        pieces = [
            z_shift(by_block[:, k].reshape(y_size * rows, VALUE), -k) for k in range(z_size)
        ]
        own, sent = call(
            functools.partial(branch_kernel, ways, z_size, rows),
            [((rows, width), f32), (((y_size - 1) * rows, width), bf16)],
            [place, *pieces, *weights],
            [SMEM] + [VMEM] * (len(pieces) + len(weights)),
            flops=2 * y_size * rows * z_size * VALUE * width,
            name="branch",
        )
        total = own
        for j in range(1, y_size):
            total = total + y_shift(sent[(j - 1) * rows : j * rows], -j).astype(f32)
        return (latents.astype(f32) + full_terms[4] * total).astype(bf16)

    return shards


def solution(mesh):
    in_specs = (
        P(("sp", "tp"), None),
        P("sp", None),
        P("sp"),
        P("sp"),
        P(),
        P("sp", "tp"),
        P("sp", "tp"),
        P("sp", "tp"),
        P(None, "tp"),
        P(None, "tp"),
        P(None, "tp"),
        P("tp"),
        P(),
        P("tp", None),
    )
    out_specs = P(("sp", "tp"), None)
    shards = make_shards(mesh.shape["sp"], mesh.shape["tp"])
    return jax.shard_map(shards, mesh=mesh, in_specs=in_specs, out_specs=out_specs, check_vma=False)
```
